256 devices in a mesh: ep: 64 (over z, y, core), tp: 4 (over x).
Axes of the slice: x: 4, y: 4, z: 8, core: 2. Of those that a mesh axis runs over, the one named last changes fastest.
Arguments:
- tokens: bfloat16 [16384, 2048], P('ep'), may hold values from -6 to 6
- norm_gain: float32 [2048], replicated, may hold values from 0.1 to 1.9
- expert_ids: int32 [16384, 2], P('ep'), may hold values from 0 to 31, all different within a row; in each aligned block of 256 rows (0 to 255, 256 to 511, ...) at most 20 rows name the same one
- route_weight: float32 [16384, 2], P('ep'), may hold values from 0.2 to 1
- w_gate: bfloat16 [64, 2048, 3584], P('ep', None, 'tp'), may hold values from -0.125 to 0.125
- w_up: bfloat16 [64, 2048, 3584], P('ep', None, 'tp'), may hold values from -0.125 to 0.125
- w_down: bfloat16 [64, 3584, 2048], P('ep', 'tp'), may hold values from -0.0625 to 0.0625
Outputs:
- mixed: bfloat16 [16384, 2048], P('ep', 'tp')
The draws below stay inside these ranges and needn't reach their ends.
Inputs may be any that keep to these rules, and one draw needn't show every extreme that they name: `expert_ids`: A token names 2 different experts. In each aligned block of 256 tokens (the tokens of one index of ep) no expert is named by more than 20 tokens, a bound that some block reaches.
All inputs are finite; a program needn't handle non-finite values.
Results may differ from the reference program's by a relative error of at most 0.014.
Values may be sent and summed in bfloat16 or wider, within the bound.
A program may use at most 128 MiB of HBM per device.

```python
import math
import jax
import jax.numpy as jnp
import numpy as np
from jax import lax

D = 2048
FF = 7168
TOP = 2
HALVES = 2
TOK_DEV = 256
EXPERTS = 32
HALF_FF = 3584
BLOCK_H = 896
CAP = 20
TOKENS = 16384
N_EP = 64
N_TP = 4


def steps_of(key, dims, pieces, smallest, top_value):
    loudness = 1.0
    for axis_at, shards_of in pieces:
        heights = jax.random.uniform(jax.random.fold_in(jax.random.fold_in(key, 6), axis_at), (shards_of,), jnp.float32, smallest / len(pieces), top_value / len(pieces))
        loudness = loudness * jnp.repeat(jnp.exp(heights), dims[axis_at] // shards_of).reshape((-1,) + (1,) * (len(dims) - 1 - axis_at))
    return loudness


def assign_block(rng, own, number, rows, number_of, top, bound, slope):
    sequence = jax.random.permutation(rng, number_of)
    packed, ordinary = shares(number_of, rows * top, bound, slope, True), shares(number_of, rows * top, bound, slope, False)
    places = jnp.arange(number_of)

    def named(tallies, offset_by):
        used = int((tallies > 0).sum())
        fixed = max(1, used // 4)
        shifted = fixed + (places - fixed + offset_by * (used - fixed)) % max(1, number_of - fixed)
        return jnp.zeros((number_of,), jnp.int32).at[sequence[jnp.where(places < fixed, places, shifted)]].set(jnp.asarray(tallies, jnp.int32))

    tallies = jnp.where(number % 4 == 0, named(packed, number // 4), named(ordinary, number - number // 4 - 1))
    mixed = jax.random.permutation(jax.random.fold_in(own, 3), number_of)
    donor, receiver = mixed[0:number_of // 2 * 2:2], mixed[1:number_of // 2 * 2:2]
    room = jnp.minimum(tallies[donor] - 1, bound - tallies[receiver]) // 2
    room = jnp.where((donor == sequence[0]) | (receiver == sequence[0]) | (tallies[receiver] == 0), 0, jnp.maximum(room, 0))
    shifted = jax.random.randint(jax.random.fold_in(own, 4), (number_of // 2,), 0, 1 << 20) % (room + 1)
    tallies = tallies.at[donor].add(-shifted).at[receiver].add(shifted)
    members = jnp.searchsorted(jnp.cumsum(tallies), jnp.arange(rows * top), side="right").astype(jnp.int32)
    table = members.reshape(top, rows).T
    table = table[jax.random.permutation(jax.random.fold_in(own, 1), rows)]
    offset_by = jax.random.randint(jax.random.fold_in(own, 2), (rows, 1), 0, top)
    return jnp.take_along_axis(table, (jnp.arange(top)[None, :] + offset_by) % top, axis=1)


def shares(count, total, reach, skew, full):
    portions = [(1 << 20) // math.isqrt(grade ** skew) + 1 for grade in range(1, count + 1)]
    largest = reach if full else min(reach, max(-(-total // count), total * portions[0] // sum(portions)))
    least = 1 if total - largest >= count - 1 else 0
    holding, surplus = [largest] + [least] * (count - 1), total - largest - least * (count - 1)
    while surplus > 0:
        movable = [i for i in range(1, count) if holding[i] < largest] or [i for i in range(1, count) if holding[i] < reach]
        mass, remaining = sum([portions[i] for i in movable]), surplus
        for i in movable:
            addition = min(reach - holding[i], max(1, remaining * portions[i] // mass), surplus)
            holding[i] = holding[i] + addition
            surplus = surplus - addition
    return np.array(holding)


def normal_values(own_key, extent, scale, most, split=(), kind=jnp.bfloat16):
    gain = steps_of(own_key, extent, split, -0.22, 0.18) if split else 1.0
    entries = jax.random.normal(own_key, extent, jnp.float32) * scale * gain
    return jnp.minimum(jnp.maximum(entries, -most), most).astype(kind)


def setup_inputs(seed: int = 0) -> dict:
    key_list = jax.random.split(jax.random.key(seed), 8)
    tokens = normal_values(key_list[0], (TOKENS, D), 1.0, 6.0, ((0, 64),))
    norm_gain = jnp.clip(1.0 + 0.18 * jax.random.normal(key_list[1], (D,), jnp.float32), 0.1, 1.9)
    expert_ids_keys = jax.random.split(jax.random.fold_in(key_list[2], 1), TOKENS // TOK_DEV)
    expert_ids_turns = jax.random.permutation(jax.random.fold_in(key_list[2], 3), TOKENS // TOK_DEV)
    expert_ids = jax.vmap(lambda own, number: assign_block(jax.random.fold_in(key_list[2], 2), own, number, TOK_DEV, EXPERTS, TOP, CAP, 1))(expert_ids_keys, expert_ids_turns).reshape((TOKENS, TOP))
    route_weight = jnp.clip(0.2 + 0.8 * jax.random.uniform(key_list[3], (TOKENS, TOP), jnp.float32) ** steps_of(key_list[3], (TOKENS, TOP), ((0, 64),), -0.2, 0.2), 0.2, 1.0)
    w_gate = normal_values(key_list[4], (EXPERTS * HALVES, D, HALF_FF), D ** -0.5, 0.125, ((0, 64), (2, 4)))
    w_up = normal_values(key_list[5], (EXPERTS * HALVES, D, HALF_FF), D ** -0.5, 0.125, ((0, 64), (2, 4)))
    w_down = normal_values(key_list[6], (EXPERTS * HALVES, HALF_FF, D), FF ** -0.5, 0.0625, ((0, 64), (1, 4)))
    return {"tokens": tokens, "norm_gain": norm_gain, "expert_ids": expert_ids, "route_weight": route_weight, "w_gate": w_gate, "w_up": w_up, "w_down": w_down}


EPSILON = 1e-05

def layer_normed(tokens, norm_gain):
    values = tokens.astype(jnp.float32)
    center = values - lax.optimization_barrier(jnp.mean(values, axis=-1, keepdims=True))
    spread = lax.optimization_barrier(jnp.mean(center * center, axis=-1, keepdims=True))
    return (center * lax.rsqrt(spread + EPSILON) * norm_gain).astype(jnp.bfloat16)

def slot_numbers(chosen, experts):
    onehot = (chosen[..., None] == jnp.arange(experts, dtype=jnp.int32)).astype(jnp.int32)
    before = jnp.cumsum(onehot, axis=1) - onehot
    return lax.optimization_barrier(jnp.sum(before * onehot, axis=-1)).astype(jnp.int32)

def reference(tokens, norm_gain, expert_ids, route_weight, w_gate, w_up, w_down):
    normed = layer_normed(tokens, norm_gain)
    padded = jnp.concatenate([normed, jnp.zeros((1, D), jnp.bfloat16)], axis=0)
    pair_count = TOK_DEV * TOP
    slots = slot_numbers(expert_ids.reshape(N_EP, pair_count), EXPERTS).reshape(-1)
    flat_expert = expert_ids.reshape(-1).astype(jnp.int32)
    index = jnp.arange(TOKENS * TOP, dtype=jnp.int32)
    source = index // pair_count
    owner = index // TOP
    place = (flat_expert * N_EP + source) * CAP + slots
    table = jnp.full((EXPERTS * N_EP * CAP,), TOKENS, jnp.int32).at[place].set(owner)
    table = table.reshape(EXPERTS, N_EP * CAP)

    def one_expert(expert):
        rows = padded[table[expert]]
        total = jnp.zeros((N_EP * CAP, D), jnp.float32)
        for half in range(HALVES):
            which = expert * HALVES + half
            gate = jnp.dot(rows, w_gate[which], preferred_element_type=jnp.float32)
            up = jnp.dot(rows, w_up[which], preferred_element_type=jnp.float32)
            hidden = (jax.nn.silu(gate) * up).astype(jnp.bfloat16)
            blocks = hidden.reshape(N_EP * CAP, N_TP, BLOCK_H).astype(jnp.float32)
            down = w_down[which].reshape(N_TP, BLOCK_H, D).astype(jnp.float32)
            block_out = jnp.einsum('rnb,nbd->nrd', blocks, down).astype(jnp.bfloat16)
            half_out = lax.optimization_barrier(jnp.sum(block_out.astype(jnp.float32), axis=0)).astype(jnp.bfloat16)
            total = total + half_out.astype(jnp.float32)
        return total
    results = lax.map(one_expert, jnp.arange(EXPERTS, dtype=jnp.int32))
    merged = results.reshape(EXPERTS * N_EP * CAP, D)
    picked = merged[place].reshape(TOKENS, TOP, D)
    return lax.optimization_barrier(jnp.sum(route_weight[:, :, None] * picked, axis=1)).astype(jnp.bfloat16)
```

```python
import jax
import jax.numpy as jnp
from jax import lax
from jax.experimental import pallas as pl
from jax.experimental.pallas import tpu as pltpu
from jax.sharding import PartitionSpec as P

MESH = pl.DeviceIdType.MESH
F32, BF16, I32 = jnp.float32, jnp.bfloat16, jnp.int32
EPSILON = 1e-05

NZ, NY, NX = 8, 4, 4
EXPERTS = NZ * NY
TOK = 256
D = 2048
CAP = 20
LANES = 128
DQ = D // NX
NJ = DQ // LANES
SLAB = CAP * NJ
BLOCK_H = 896
NT = BLOCK_H // LANES

GROUPS = ((1, 7), (0, 4), (2, 6), (3, 5))
NG = len(GROUPS)
PER = len(GROUPS[0])
HALF = PER * NY * CAP
ROWS = 2 * HALF
QUARTERS = (2, 1, 3, 0)


def place_numbers(ids):
    lanes = lax.broadcasted_iota(I32, (TOK, LANES), 1)
    named = [ids[:, k : k + 1] == lanes for k in range(2)]
    counts = (named[0].astype(F32) + named[1].astype(F32)).astype(BF16)
    rows = lax.broadcasted_iota(I32, (TOK, TOK), 0)
    cols = lax.broadcasted_iota(I32, (TOK, TOK), 1)
    earlier = jnp.where(cols < rows, 1.0, 0.0).astype(BF16)
    before = jnp.dot(earlier, counts, preferred_element_type=F32)
    slots = [jnp.sum(jnp.where(m, before, 0.0), axis=1, keepdims=True).astype(I32) for m in named]
    return [ids[:, k : k + 1] * CAP + slots[k] for k in range(2)]


def pre_kernel(tok_ref, gain_ref, ids_ref, out_ref, rows_ref, slab_ref):
    x = lax.axis_index("tp")
    columns = pl.ds(pl.multiple_of(x * DQ, DQ), DQ)
    values = tok_ref[...].astype(F32)
    mean = jnp.mean(values, axis=-1, keepdims=True)
    center = values - mean
    spread = jnp.mean(center * center, axis=-1, keepdims=True)
    quarter = tok_ref[:, columns].astype(F32) - mean
    normed = (quarter * lax.rsqrt(spread + EPSILON) * gain_ref[:, columns]).astype(BF16)
    place = place_numbers(ids_ref[...])
    cols = lax.broadcasted_iota(I32, (TOK, EXPERTS * CAP), 1)
    chosen = jnp.where((cols == place[0]) | (cols == place[1]), 1.0, 0.0).astype(BF16)
    rows_ref[...] = lax.dot_general(
        chosen, normed, (((0,), (0,)), ((), ())), preferred_element_type=F32
    )
    for e in range(EXPERTS):
        for j in range(NJ):
            slab_ref[pl.ds(e * SLAB + j * CAP, CAP), :] = rows_ref[
                pl.ds(e * CAP, CAP), pl.ds(j * LANES, LANES)
            ]
    out_ref[...] = slab_ref[...].reshape(EXPERTS, SLAB, LANES).astype(BF16)


def post_kernel(back_ref, ids_ref, weight_ref, out_ref, slab_ref, rows_ref):
    slab_ref[...] = back_ref[...].reshape(EXPERTS * SLAB, LANES).astype(F32)
    for e in range(EXPERTS):
        for j in range(NJ):
            rows_ref[pl.ds(e * CAP, CAP), pl.ds(j * LANES, LANES)] = slab_ref[
                pl.ds(e * SLAB + j * CAP, CAP), :
            ]
    rows = rows_ref[...].astype(BF16)
    place = place_numbers(ids_ref[...])
    cols = lax.broadcasted_iota(I32, (TOK, EXPERTS * CAP), 1)
    total = jnp.zeros((TOK, DQ), F32)
    for k in range(2):
        chosen = jnp.where(cols == place[k], 1.0, 0.0).astype(BF16)
        picked = jnp.dot(chosen, rows, preferred_element_type=F32)
        total = total + weight_ref[:, k : k + 1] * picked
    out_ref[...] = total.astype(BF16)


def main_kernel(
    out_slabs, wg_hbm, wu_hbm, wd_hbm, result,
    wgu, wd, arrived, routed, hidden, slabs, rows,
    own, psend, precv, t1, u1, t2, u2, ysend, back,
    w_sem, d_send, d_recv, ag_send, ag_recv, p_send, p_recv,
    r1_send, r1_recv, r2_send, r2_recv, y_send, y_recv,
):
    x = lax.axis_index("tp")
    ep = lax.axis_index("ep")
    core = lax.rem(ep, 2)
    expert = ep // 2
    y = lax.rem(expert, NY)
    z = expert // NY
    right, left = {"tp": lax.rem(x + 1, NX)}, {"tp": lax.rem(x + NX - 1, NX)}
    partner = {"ep": ep + 1 - 2 * core}

    def chip(to_z, to_y):
        return {"ep": (to_z * NY + to_y) * 2 + core}

    def remote(src, dst, send, recv, device):
        return pltpu.make_async_remote_copy(
            src_ref=src, dst_ref=dst, send_sem=send, recv_sem=recv,
            device_id=device, device_id_type=MESH,
        )

    def weight_copies():
        copies = []
        for n in range(NT):
            tile = pl.ds(n * LANES, LANES)
            for k, w in enumerate((wg_hbm, wu_hbm)):
                copies.append(
                    pltpu.make_async_copy(
                        w.at[0, :, tile], wgu.at[n, :, pl.ds(k * LANES, LANES)], w_sem.at[2 * n + k]
                    )
                )
        copies.append(pltpu.make_async_copy(wd_hbm.at[0], wd, w_sem.at[2 * NT]))
        return copies

    for copy in weight_copies():
        copy.start()

    barrier = pltpu.get_barrier_semaphore()

    def greet(i, carry):
        other = lax.rem(expert + i, EXPERTS)
        pl.semaphore_signal(
            barrier, inc=1, device_id={"ep": other * 2 + core}, device_id_type=MESH
        )
        return carry

    lax.fori_loop(1, EXPERTS, greet, 0)
    for device in (right, left, partner):
        pl.semaphore_signal(barrier, inc=1, device_id=device, device_id_type=MESH)
    pl.semaphore_wait(barrier, EXPERTS - 1 + 3)

    for g, offsets in enumerate(GROUPS):
        for d, dz in enumerate(offsets):
            to_z = lax.rem(z + dz, NZ)
            for dy in range(NY):
                to_y = lax.rem(y + dy, NY)
                if dz == 0 and dy == 0:
                    continue
                remote(
                    out_slabs.at[to_z * NY + to_y], arrived.at[g, d, y],
                    d_send, d_recv.at[g], chip(to_z, to_y),
                ).start()
            if dz == 0:
                arrived[g, d, y] = out_slabs[expert]

    def wait_slabs(sem, count, recv):
        span = pl.ds(0, count)
        copy = remote(out_slabs.at[span], back.at[span], sem, sem, partner)
        copy.wait_recv() if recv else copy.wait_send()

    def quarter_columns(q):
        return pl.ds(pl.multiple_of(q * DQ, DQ), DQ)

    q_own, q_left, q_right, q_far = (
        x, lax.rem(x + NX - 1, NX), lax.rem(x + 1, NX), lax.rem(x + 2, NX)
    )

    own_rows, other_rows = pl.ds(0, HALF), pl.ds(HALF, HALF)
    first, second = pl.ds(0, HALF // 2), pl.ds(HALF // 2, HALF // 2)

    def gather_copy(g, index):
        q, span, device = (
            (q_own, own_rows, right),
            (q_own, own_rows, left),
            (q_left, first, right),
            (q_right, second, left),
            (q_own, None, partner),
            (q_left, None, partner),
            (q_right, None, partner),
            (q_far, None, partner),
        )[index]
        columns = quarter_columns(q)
        src = routed.at[g, own_rows if span is None else span, columns]
        dst = routed.at[g, other_rows if span is None else span, columns]
        return remote(src, dst, ag_send.at[g, index], ag_recv.at[g, index], device)

    def gather_start(g):
        wait_slabs(d_recv.at[g], PER * NY - (1 if 0 in GROUPS[g] else 0), True)
        slabs[...] = arrived[g].reshape(PER * NY * SLAB, LANES).astype(F32)
        for i in range(PER * NY):
            for j in range(NJ):
                rows[pl.ds(i * CAP, CAP), pl.ds(j * LANES, LANES)] = slabs[
                    pl.ds(i * SLAB + j * CAP, CAP), :
                ]
        routed[g, own_rows, quarter_columns(q_own)] = rows[...].astype(BF16)
        for index in (0, 1, 4):
            gather_copy(g, index).start()

    def gather_forward(g):
        gather_copy(g, 0).wait_recv()
        gather_copy(g, 2).start()
        gather_copy(g, 5).start()
        gather_copy(g, 1).wait_recv()
        gather_copy(g, 3).start()
        gather_copy(g, 6).start()

    def gather_finish(g):
        gather_copy(g, 2).wait_recv()
        gather_copy(g, 3).wait_recv()
        gather_copy(g, 7).start()

    def gather_partner(g):
        for index in range(4, 8):
            gather_copy(g, index).wait_recv()

    def up_part(g):
        def step(n, carry):
            both = jnp.dot(routed[g], wgu[n], preferred_element_type=F32)
            gate, up = both[:, :LANES], both[:, LANES:]
            value = gate / (1.0 + jnp.exp(-gate)) * up
            hidden[:, pl.ds(pl.multiple_of(n * LANES, LANES), LANES)] = value.astype(BF16)
            return carry

        lax.fori_loop(0, NT, step, 0)

    def partial_copy(g, k):
        return remote(
            psend.at[g, k], precv.at[g, k], p_send.at[g, k], p_recv.at[g, k], partner
        )

    def down_part(g):
        for k, off in enumerate(QUARTERS):
            value = jnp.dot(
                hidden[...], wd[:, quarter_columns(lax.rem(x + off, NX))],
                preferred_element_type=F32,
            )
            psend[g, k] = value[HALF:].astype(BF16)
            own[g, k] = value[:HALF]
            partial_copy(g, k).start()

    def first_copy(g, way):
        span = (first, second)[way]
        return remote(
            t1.at[g, span], u1.at[g, span], r1_send.at[g, way], r1_recv.at[g, way], (right, left)[way]
        )

    def second_copy(g, way):
        return remote(
            t2.at[g, way], u2.at[g, way], r2_send.at[g, way], r2_recv.at[g, way], (right, left)[way]
        )

    def reduce_first(g):
        partial_copy(g, 0).wait_recv()
        t1[g] = (own[g, 0] + precv[g, 0].astype(F32)).astype(BF16)
        for way in range(2):
            first_copy(g, way).start()

    def reduce_second(g):
        for way, spans in enumerate(((first, second), (second, first))):
            partial_copy(g, 1 + way).wait_recv()
            first_copy(g, way).wait_recv()
            added, plain = spans
            t2[g, way, added] = (
                own[g, 1 + way, added] + precv[g, 1 + way, added].astype(F32)
                + u1[g, added].astype(F32)
            ).astype(BF16)
            t2[g, way, plain] = (
                own[g, 1 + way, plain] + precv[g, 1 + way, plain].astype(F32)
            ).astype(BF16)
            second_copy(g, way).start()

    def reduce_last(g):
        partial_copy(g, 3).wait_recv()
        second_copy(g, 0).wait_recv()
        second_copy(g, 1).wait_recv()
        rows[...] = (
            own[g, 3] + precv[g, 3].astype(F32) + u2[g, 0].astype(F32) + u2[g, 1].astype(F32)
        )
        for i in range(PER * NY):
            for j in range(NJ):
                slabs[pl.ds(i * SLAB + j * CAP, CAP), :] = rows[
                    pl.ds(i * CAP, CAP), pl.ds(j * LANES, LANES)
                ]
        ysend[g] = slabs[...].reshape(PER, NY, SLAB, LANES).astype(BF16)
        for d, dz in enumerate(GROUPS[g]):
            to_z = lax.rem(z + NZ - dz, NZ)
            for dy in range(NY):
                to_y = lax.rem(y + dy, NY)
                if dz == 0 and dy == 0:
                    back[expert] = ysend[g, d, y]
                    continue
                remote(
                    ysend.at[g, d, to_y], back.at[expert], y_send, y_recv, chip(to_z, to_y)
                ).start()

    gather_start(0)
    gather_start(1)
    gather_forward(0)
    gather_start(2)
    gather_finish(0)
    gather_forward(1)
    gather_start(3)
    for copy in weight_copies():
        copy.wait()
    gather_partner(0)
    up_part(0)
    gather_finish(1)
    gather_forward(2)
    down_part(0)
    gather_finish(2)
    gather_forward(3)
    gather_partner(1)
    up_part(1)
    reduce_first(0)
    gather_finish(3)
    down_part(1)
    reduce_second(0)
    gather_partner(2)
    up_part(2)
    reduce_first(1)
    reduce_last(0)
    down_part(2)
    reduce_second(1)
    gather_partner(3)
    up_part(3)
    reduce_first(2)
    reduce_last(1)
    down_part(3)
    reduce_second(2)
    reduce_first(3)
    reduce_last(2)
    reduce_second(3)
    reduce_last(3)

    wait_slabs(d_send, EXPERTS - 1, False)
    for g in range(NG):
        for index in range(8):
            gather_copy(g, index).wait_send()
        for k in range(4):
            partial_copy(g, k).wait_send()
        for way in range(2):
            first_copy(g, way).wait_send()
            second_copy(g, way).wait_send()
    wait_slabs(y_send, EXPERTS - 1, False)
    wait_slabs(y_recv, EXPERTS - 1, True)
    result[...] = back[...]


def body(tokens, norm_gain, expert_ids, route_weight, w_gate, w_up, w_down):
    vmem = pl.BlockSpec(memory_space=pltpu.VMEM)
    hbm = pl.BlockSpec(memory_space=pl.ANY)
    slab_array = jax.ShapeDtypeStruct((EXPERTS, SLAB, LANES), BF16)
    params = dict(vmem_limit_bytes=60 * 1024 * 1024)
    out_slabs = pl.pallas_call(
        pre_kernel,
        out_shape=slab_array,
        in_specs=[vmem] * 3,
        out_specs=vmem,
        scratch_shapes=[
            pltpu.VMEM((EXPERTS * CAP, DQ), F32),
            pltpu.VMEM((EXPERTS * SLAB, LANES), F32),
        ],
        compiler_params=pltpu.CompilerParams(**params),
    )(tokens, norm_gain.reshape(1, D), expert_ids)

    dma = pltpu.SemaphoreType.DMA
    returned = pl.pallas_call(
        main_kernel,
        out_shape=slab_array,
        in_specs=[vmem, hbm, hbm, hbm],
        out_specs=vmem,
        scratch_shapes=[
            pltpu.VMEM((NT, D, 2 * LANES), BF16),
            pltpu.VMEM((BLOCK_H, D), BF16),
            pltpu.VMEM((NG, PER, NY, SLAB, LANES), BF16),
            pltpu.VMEM((NG, ROWS, D), BF16),
            pltpu.VMEM((ROWS, BLOCK_H), BF16),
            pltpu.VMEM((PER * NY * SLAB, LANES), F32),
            pltpu.VMEM((HALF, DQ), F32),
            pltpu.VMEM((NG, 4, HALF, DQ), F32),
            pltpu.VMEM((NG, 4, HALF, DQ), BF16),
            pltpu.VMEM((NG, 4, HALF, DQ), BF16),
            pltpu.VMEM((NG, HALF, DQ), BF16),
            pltpu.VMEM((NG, HALF, DQ), BF16),
            pltpu.VMEM((NG, 2, HALF, DQ), BF16),
            pltpu.VMEM((NG, 2, HALF, DQ), BF16),
            pltpu.VMEM((NG, PER, NY, SLAB, LANES), BF16),
            pltpu.VMEM((EXPERTS, SLAB, LANES), BF16),
            dma((2 * NT + 1,)),
            dma,
            dma((NG,)),
            dma((NG, 8)),
            dma((NG, 8)),
            dma((NG, 4)),
            dma((NG, 4)),
            dma((NG, 2)),
            dma((NG, 2)),
            dma((NG, 2)),
            dma((NG, 2)),
            dma,
            dma,
        ],
        compiler_params=pltpu.CompilerParams(
            collective_id=0, has_side_effects=True, **params
        ),
    )(out_slabs, w_gate, w_up, w_down)

    return pl.pallas_call(
        post_kernel,
        out_shape=jax.ShapeDtypeStruct((TOK, DQ), BF16),
        in_specs=[vmem] * 3,
        out_specs=vmem,
        scratch_shapes=[
            pltpu.VMEM((EXPERTS * SLAB, LANES), F32),
            pltpu.VMEM((EXPERTS * CAP, DQ), F32),
        ],
        compiler_params=pltpu.CompilerParams(**params),
    )(returned, expert_ids, route_weight)


def solution(mesh):
    in_specs = (
        P("ep", None),
        P(),
        P("ep", None),
        P("ep", None),
        P("ep", None, "tp"),
        P("ep", None, "tp"),
        P("ep", "tp", None),
    )
    return jax.shard_map(
        body, mesh=mesh, in_specs=in_specs, out_specs=P("ep", "tp"), check_vma=False
    )
```

```python
import jax
import jax.numpy as jnp
from jax import lax
from jax.experimental import pallas as pl
from jax.experimental.pallas import tpu as pltpu
from jax.sharding import PartitionSpec as P

MESH = pl.DeviceIdType.MESH
F32, BF16, I32 = jnp.float32, jnp.bfloat16, jnp.int32
EPSILON = 1e-05

NZ, NY, NX = 8, 4, 4
EXPERTS = NZ * NY
TOK = 256
D = 2048
CAP = 20
LANES = 128
DQ = D // NX
NJ = DQ // LANES
SLAB = CAP * NJ
BLOCK_H = 896
NT = BLOCK_H // LANES
BLK = NY * CAP

GROUPS = ((2,), (5,), (7,), (4,), (3,), (6,), (1,), (0,))
ISSUE = (0, 3, 1, 4, 7, 5, 2, 6)
WHOLE = (2, 6, 7)
COMBINE = (0, 1, 2, 3, 4, 5, 6, 7)
ORDER = (
    ("start", 0),
    ("start", 1),
    ("forward", 0),
    ("start", 7),
    ("forward", 1),
    ("start", 5),
    ("finish", 0),
    ("weights",),
    ("ready", 0),
    ("up", 0, 0),
    ("start", 3),
    ("up", 0, 1),
    ("up", 0, 2),
    ("finish", 1),
    ("up", 0, 3),
    ("down", 0, 0),
    ("down", 0, 1),
    ("down", 0, 2),
    ("down", 0, 3),
    ("forward", 5),
    ("first", 0),
    ("ready", 1),
    ("up", 1, 0),
    ("start", 2),
    ("up", 1, 1),
    ("forward", 3),
    ("up", 1, 2),
    ("start", 4),
    ("up", 1, 3),
    ("down", 1, 0),
    ("down", 1, 1),
    ("down", 1, 2),
    ("down", 1, 3),
    ("finish", 5),
    ("first", 1),
    ("ready", 2),
    ("up", 2, 0),
    ("second", 0),
    ("up", 2, 1),
    ("up", 2, 2),
    ("finish", 3),
    ("up", 2, 3),
    ("down", 2, 0),
    ("down", 2, 1),
    ("down", 2, 2),
    ("forward", 4),
    ("down", 2, 3),
    ("first", 2),
    ("ready", 3),
    ("up", 3, 0),
    ("second", 1),
    ("start", 6),
    ("up", 3, 1),
    ("up", 3, 2),
    ("last", 0),
    ("up", 3, 3),
    ("down", 3, 0),
    ("down", 3, 1),
    ("finish", 4),
    ("down", 3, 2),
    ("down", 3, 3),
    ("first", 3),
    ("second", 2),
    ("ready", 4),
    ("up", 4, 0),
    ("up", 4, 1),
    ("up", 4, 2),
    ("last", 1),
    ("up", 4, 3),
    ("down", 4, 0),
    ("down", 4, 1),
    ("down", 4, 2),
    ("second", 3),
    ("down", 4, 3),
    ("first", 4),
    ("ready", 5),
    ("up", 5, 0),
    ("up", 5, 1),
    ("last", 2),
    ("up", 5, 2),
    ("up", 5, 3),
    ("down", 5, 0),
    ("down", 5, 1),
    ("down", 5, 2),
    ("down", 5, 3),
    ("ready", 6),
    ("up", 6, 0),
    ("first", 5),
    ("last", 3),
    ("up", 6, 1),
    ("second", 4),
    ("up", 6, 2),
    ("up", 6, 3),
    ("down", 6, 0),
    ("down", 6, 1),
    ("down", 6, 2),
    ("down", 6, 3),
    ("ready", 7),
    ("up", 7, 0),
    ("second", 5),
    ("first", 6),
    ("up", 7, 1),
    ("up", 7, 2),
    ("up", 7, 3),
    ("last", 4),
    ("down", 7, 0),
    ("down", 7, 1),
    ("down", 7, 2),
    ("down", 7, 3),
    ("first", 7),
    ("last", 5),
    ("second", 6),
    ("second", 7),
    ("last", 6),
    ("mix", 0),
    ("mix", 1),
    ("mix", 2),
    ("mix", 3),
    ("mix", 4),
    ("last", 7),
    ("mix", 5),
    ("mix", 6),
    ("mix", 7),
)
NG = len(GROUPS)
OFFSETS = tuple(dz for offsets in GROUPS for dz in offsets)
BASE = tuple(sum(len(o) for o in GROUPS[:g]) for g in range(NG))
SIZE = tuple(len(o) for o in GROUPS)
NF = len(WHOLE)
GATHERED = tuple(g for g in range(NG) if g not in WHOLE)
TOP_ROWS = 2 * BLK * max(SIZE)
CUTS = (0, 2, 4, 6, 7)
QUARTERS = (2, 1, 3, 0)
ALL_ROWS = EXPERTS * CAP
VMEM_BYTES = 53 * 1024 * 1024 + 256 * 1024


def main_kernel(
    tok_hbm, gain_ref, ids_ref, weight_ref, wg_hbm, wu_hbm, wd_hbm, result,
    tok, normed, full_slabs, full_in, out_slabs, arrived, mix_hi, mix_lo,
    wgu, wd, routed, acc, hidden, rows, slabs,
    own, psend, precv, t1, u1, t2, u2, ysend, back, total,
    tok_sem, w_sem, f_send, d_send, d_recv, ag_send, ag_recv, p_send, p_recv,
    r1_send, r1_recv, r2_send, r2_recv, y_send, y_recv,
):
    x = lax.axis_index("tp")
    ep = lax.axis_index("ep")
    core = lax.rem(ep, 2)
    expert = ep // 2
    y = lax.rem(expert, NY)
    z = expert // NY
    right, left = {"tp": lax.rem(x + 1, NX)}, {"tp": lax.rem(x + NX - 1, NX)}
    partner = {"ep": ep + 1 - 2 * core}

    def chip(to_z, to_y):
        return {"ep": (to_z * NY + to_y) * 2 + core}

    def remote(src, dst, send, recv, device):
        return pltpu.make_async_remote_copy(
            src_ref=src, dst_ref=dst, send_sem=send, recv_sem=recv,
            device_id=device, device_id_type=MESH,
        )

    def weight_copies():
        copies = []
        for n in range(NT):
            tile = pl.ds(n * LANES, LANES)
            for k, w in enumerate((wg_hbm, wu_hbm)):
                copies.append(
                    pltpu.make_async_copy(
                        w.at[0, :, tile], wgu.at[n, :, pl.ds(k * LANES, LANES)], w_sem.at[0]
                    )
                )
        copies.append(pltpu.make_async_copy(wd_hbm.at[0], wd, w_sem.at[1]))
        return copies

    tok_copy = pltpu.make_async_copy(tok_hbm, tok, tok_sem)
    tok_copy.start()

    barrier = pltpu.get_barrier_semaphore()

    def greet(i, carry):
        other = lax.rem(expert + i, EXPERTS)
        pl.semaphore_signal(
            barrier, inc=1, device_id={"ep": other * 2 + core}, device_id_type=MESH
        )
        return carry

    lax.fori_loop(1, EXPERTS, greet, 0)
    for device in (right, left, partner):
        pl.semaphore_signal(barrier, inc=1, device_id=device, device_id_type=MESH)
    for copy in weight_copies():
        copy.start()

    def rows_wait(sem, count, recv):
        copy = remote(t1.at[pl.ds(0, count)], u1.at[pl.ds(0, count)], sem, sem, partner)
        copy.wait_recv() if recv else copy.wait_send()

    def quarter_columns(q):
        return pl.ds(pl.multiple_of(q * DQ, DQ), DQ)

    ids = [ids_ref[k : k + 1, :] for k in range(2)]
    experts = lax.broadcasted_iota(I32, (EXPERTS, TOK), 0)
    named = [experts == ids[k] for k in range(2)]
    counts = (named[0].astype(F32) + named[1].astype(F32)).astype(BF16)
    token_from = lax.broadcasted_iota(I32, (TOK, TOK), 0)
    token_to = lax.broadcasted_iota(I32, (TOK, TOK), 1)
    earlier = jnp.where(token_from < token_to, 1.0, 0.0).astype(BF16)
    before = jnp.dot(counts, earlier, preferred_element_type=F32)
    place = []
    for k in range(2):
        slot = jnp.sum(jnp.where(named[k], before, 0.0), axis=0, keepdims=True).astype(I32)
        away = ((ids[k] >> 2) + (NZ - z)) & (NZ - 1)
        position = jnp.zeros_like(away)
        for at, dz in enumerate(OFFSETS):
            position = jnp.where(away == dz, at, position)
        place.append((position * NY + (ids[k] & (NY - 1))) * CAP + slot)
    row_index = lax.broadcasted_iota(I32, (ALL_ROWS, TOK), 0)
    hits = [row_index == place[k] for k in range(2)]
    chosen = jnp.where(hits[0] | hits[1], 1.0, 0.0).astype(BF16)

    tok_copy.wait()
    values = tok[...].astype(F32)
    center = values - jnp.mean(values, axis=-1, keepdims=True)
    spread = jnp.mean(center * center, axis=-1, keepdims=True)
    normed[...] = (center * lax.rsqrt(spread + EPSILON) * gain_ref[...]).astype(BF16)

    rows[...] = jnp.dot(chosen, normed[:, quarter_columns(x)], preferred_element_type=F32)
    for i in range(EXPERTS):
        if i // NY in [BASE[g] for g in WHOLE]:
            continue
        for j in range(NJ):
            slabs[pl.ds(i * SLAB + j * CAP, CAP), :] = rows[
                pl.ds(i * CAP, CAP), pl.ds(j * LANES, LANES)
            ]
    for g in range(NG):
        if g not in WHOLE:
            span = pl.ds(BASE[g] * NY, SIZE[g] * NY)
            out_slabs[span] = (
                slabs[pl.ds(BASE[g] * NY * SLAB, SIZE[g] * NY * SLAB)]
                .reshape(SIZE[g] * NY, SLAB, LANES)
                .astype(BF16)
            )
    for f, g in enumerate(WHOLE):
        near = chosen[BASE[g] * BLK : (BASE[g] + 1) * BLK]
        for q in range(NX):
            rows[0:BLK] = jnp.dot(
                near, normed[:, q * DQ : (q + 1) * DQ], preferred_element_type=F32
            )
            for i in range(NY):
                for j in range(NJ):
                    slabs[pl.ds(i * SLAB + j * CAP, CAP), :] = rows[
                        pl.ds(i * CAP, CAP), pl.ds(j * LANES, LANES)
                    ]
            full_slabs[f * NY : (f + 1) * NY, q] = (
                slabs[0 : NY * SLAB].reshape(NY, SLAB, LANES).astype(BF16)
            )

    pl.semaphore_wait(barrier, EXPERTS - 1 + 3)

    for g in ISSUE:
        if g in WHOLE:
            at = WHOLE.index(g) * NY
            for dy in range(NY):
                to_y = lax.rem(y + dy, NY)
                if dy or GROUPS[g][0]:
                    remote(
                        full_slabs.at[at + to_y], full_in.at[at + y], f_send, d_recv.at[g],
                        chip(lax.rem(z + GROUPS[g][0], NZ), to_y),
                    ).start()
                else:
                    full_in[at + y] = full_slabs[at + y]
            continue
        for d, dz in enumerate(GROUPS[g]):
            for dy in range(NY):
                to_y = lax.rem(y + dy, NY)
                at = (BASE[g] + d) * NY
                if dy or dz:
                    remote(
                        out_slabs.at[at + to_y], arrived.at[at + y],
                        d_send, d_recv.at[g], chip(lax.rem(z + dz, NZ), to_y),
                    ).start()
                else:
                    arrived[at + y] = out_slabs[at + y]
    mix = jnp.where(hits[0], weight_ref[0:1, :], 0.0) + jnp.where(hits[1], weight_ref[1:2, :], 0.0)
    high = mix.astype(BF16)
    mix_hi[...] = high
    mix_lo[...] = (mix - high.astype(F32)).astype(BF16)

    def wait_slabs(sem, count, recv):
        span = pl.ds(0, count)
        copy = remote(out_slabs.at[span], back.at[span], sem, sem, partner)
        copy.wait_recv() if recv else copy.wait_send()

    q_own, q_left, q_right, q_far = (
        x, lax.rem(x + NX - 1, NX), lax.rem(x + 1, NX), lax.rem(x + 2, NX)
    )

    def parts_of(g):
        count = SIZE[g] * BLK
        cut = -(-count // 32) * 16
        return (0, cut), (cut, count - cut)

    def shared(g, part):
        return pl.ds(BASE[g] * BLK + part[0], part[1])

    def gather_rows(g, part, other):
        start = BASE[g] * 2 * BLK + (SIZE[g] * BLK if other else 0)
        return pl.ds(start + part[0], part[1])

    def gather_copy(g, index):
        whole = (0, SIZE[g] * BLK)
        first, second = parts_of(g)
        q, part, device = (
            (q_own, whole, right),
            (q_own, whole, left),
            (q_left, first, right),
            (q_right, second, left),
            (q_own, whole, partner),
            (q_left, whole, partner),
            (q_right, whole, partner),
            (q_far, whole, partner),
        )[index]
        columns = pl.ds(0, D) if g in WHOLE else quarter_columns(q)
        src = routed.at[gather_rows(g, part, False), columns]
        dst = routed.at[gather_rows(g, part, index >= 4), columns]
        sent = 8 if g in WHOLE else index
        return remote(src, dst, ag_send.at[sent], ag_recv.at[g, (0, 1, 2, 2, 3, 3, 3, 3)[index]], device)

    def gather_start(g):
        if g in WHOLE:
            at = WHOLE.index(g) * NY
            wait_slabs(d_recv.at[g], (NY - (0 in GROUPS[g])) * NX, True)
            for q in range(NX):
                slabs[0 : NY * SLAB] = (
                    full_in[at : at + NY, q].reshape(NY * SLAB, LANES).astype(F32)
                )
                for i in range(NY):
                    for j in range(NJ):
                        rows[pl.ds(i * CAP, CAP), pl.ds(j * LANES, LANES)] = slabs[
                            pl.ds(i * SLAB + j * CAP, CAP), :
                        ]
                routed[gather_rows(g, (0, BLK), False), q * DQ : (q + 1) * DQ] = rows[
                    0:BLK
                ].astype(BF16)
            gather_copy(g, 4).start()
            return
        count = SIZE[g] * NY
        wait_slabs(d_recv.at[g], count - (0 in GROUPS[g]), True)
        span = pl.ds(BASE[g] * NY, count)
        slabs[0 : count * SLAB] = arrived[span].reshape(count * SLAB, LANES).astype(F32)
        for i in range(count):
            for j in range(NJ):
                rows[pl.ds(i * CAP, CAP), pl.ds(j * LANES, LANES)] = slabs[
                    pl.ds(i * SLAB + j * CAP, CAP), :
                ]
        routed[gather_rows(g, (0, count * CAP), False), quarter_columns(q_own)] = rows[
            0 : count * CAP
        ].astype(BF16)
        for index in (0, 1, 4):
            gather_copy(g, index).start()

    def gather_forward(g):
        gather_copy(g, 0).wait_recv()
        gather_copy(g, 2).start()
        gather_copy(g, 5).start()
        gather_copy(g, 1).wait_recv()
        gather_copy(g, 3).start()
        gather_copy(g, 6).start()

    def gather_finish(g):
        rows_wait(ag_recv.at[g, 2], SIZE[g] * BLK, True)
        gather_copy(g, 7).start()

    def gather_partner(g):
        span = gather_rows(g, (0, SIZE[g] * BLK), True)
        remote(
            routed.at[span], routed.at[span], ag_send.at[8], ag_recv.at[g, 3], partner
        ).wait_recv()

    def up_part(g, part):
        count = 2 * SIZE[g] * BLK
        span = pl.ds(BASE[g] * 2 * BLK, count)

        def activate(n):
            gate, up = acc[n % 2, 0:count, 0:LANES], acc[n % 2, 0:count, LANES:]
            value = gate / (1.0 + jnp.exp(-gate)) * up
            hidden[0:count, n * LANES : (n + 1) * LANES] = value.astype(BF16)

        for n in range(CUTS[part], CUTS[part + 1]):
            if n:
                activate(n - 1)
            acc[n % 2, 0:count] = jnp.dot(routed[span], wgu[n], preferred_element_type=F32)
        if CUTS[part + 1] == NT:
            activate(NT - 1)

    def partial_copy(g, k):
        span = shared(g, (0, SIZE[g] * BLK))
        return remote(
            psend.at[k, span], precv.at[k, span], p_send, p_recv.at[g, k], partner
        )

    def down_part(g, k):
        count = SIZE[g] * BLK
        span = shared(g, (0, count))
        value = jnp.dot(
            hidden[0 : 2 * count], wd[:, quarter_columns(lax.rem(x + QUARTERS[k], NX))],
            preferred_element_type=F32,
        )
        psend[k, span] = value[count:].astype(BF16)
        own[k, span] = value[:count]
        partial_copy(g, k).start()

    def first_copy(g, way):
        span = shared(g, parts_of(g)[way])
        return remote(
            t1.at[span], u1.at[span], r1_send, r1_recv.at[g, way], (right, left)[way]
        )

    def second_copy(g, way):
        span = shared(g, (0, SIZE[g] * BLK))
        return remote(
            t2.at[way, span], u2.at[way, span], r2_send, r2_recv.at[g],
            (right, left)[way],
        )

    def chip_sum(k, span):
        return own[k, span] + precv[k, span].astype(F32)

    def reduce_first(g):
        partial_copy(g, 0).wait_recv()
        span = shared(g, (0, SIZE[g] * BLK))
        t1[span] = chip_sum(0, span).astype(BF16)
        for way in range(2):
            first_copy(g, way).start()

    def reduce_second(g):
        for way in range(2):
            added, plain = (shared(g, parts_of(g)[p]) for p in (way, 1 - way))
            partial_copy(g, 1 + way).wait_recv()
            t2[way, plain] = chip_sum(1 + way, plain).astype(BF16)
            first_copy(g, way).wait_recv()
            t2[way, added] = (chip_sum(1 + way, added) + u1[added].astype(F32)).astype(BF16)
            second_copy(g, way).start()

    def reduce_last(g):
        count = SIZE[g] * BLK
        span = shared(g, (0, count))
        partial_copy(g, 3).wait_recv()
        remote(
            t2.at[:, span], u2.at[:, span], r2_send, r2_recv.at[g], partner
        ).wait_recv()
        rows[0:count] = chip_sum(3, span) + u2[0, span].astype(F32) + u2[1, span].astype(F32)
        for i in range(SIZE[g] * NY):
            for j in range(NJ):
                slabs[pl.ds(i * SLAB + j * CAP, CAP), :] = rows[
                    pl.ds(i * CAP, CAP), pl.ds(j * LANES, LANES)
                ]
        ysend[pl.ds(BASE[g] * NY, SIZE[g] * NY)] = (
            slabs[0 : SIZE[g] * NY * SLAB].reshape(SIZE[g] * NY, SLAB, LANES).astype(BF16)
        )
        for d, dz in enumerate(GROUPS[g]):
            at = (BASE[g] + d) * NY
            for dy in range(NY):
                to_y = lax.rem(y + dy, NY)
                if dz == 0 and dy == 0:
                    back[at + y] = ysend[at + y]
                    continue
                remote(
                    ysend.at[at + to_y], back.at[at + y], y_send, y_recv.at[g],
                    chip(lax.rem(z + NZ - dz, NZ), to_y),
                ).start()

    def combine(g):
        count = SIZE[g] * NY
        wait_slabs(y_recv.at[g], count - (0 in GROUPS[g]), True)
        slabs[0 : count * SLAB] = (
            back[pl.ds(BASE[g] * NY, count)].reshape(count * SLAB, LANES).astype(F32)
        )
        for i in range(count):
            for j in range(NJ):
                rows[pl.ds(i * CAP, CAP), pl.ds(j * LANES, LANES)] = slabs[
                    pl.ds(i * SLAB + j * CAP, CAP), :
                ]
        picked = rows[0 : count * CAP].astype(BF16)
        span = pl.ds(BASE[g] * BLK, count * CAP)
        value = sum(
            lax.dot_general(
                mix[span], picked, (((0,), (0,)), ((), ())), preferred_element_type=F32
            )
            for mix in (mix_hi, mix_lo)
        )
        if g == COMBINE[0]:
            total[...] = value
        elif g != COMBINE[-1]:
            total[...] += value
        else:
            result[...] = (total[...] + value).astype(BF16)

    def weights_wait():
        pltpu.make_async_copy(wgu, wgu, w_sem.at[0]).wait()
        pltpu.make_async_copy(wd, wd, w_sem.at[1]).wait()

    steps = {
        "start": gather_start,
        "forward": gather_forward,
        "finish": gather_finish,
        "weights": weights_wait,
        "ready": gather_partner,
        "up": up_part,
        "down": down_part,
        "first": reduce_first,
        "second": reduce_second,
        "last": reduce_last,
        "mix": combine,
    }
    for name, *which in ORDER:
        steps[name](*which)

    if NF:
        span = pl.ds(0, NF * NY - (0 in [GROUPS[g][0] for g in WHOLE]))
        remote(full_slabs.at[span], full_in.at[span], f_send, f_send, partner).wait_send()
        span = pl.ds(0, NF * BLK)
        remote(
            routed.at[span], routed.at[span], ag_send.at[8], ag_send.at[8], partner
        ).wait_send()
    gathered = sum(SIZE[g] for g in GATHERED)
    own_sent = 0 in [dz for g in GATHERED for dz in GROUPS[g]]
    wait_slabs(d_send, gathered * NY - own_sent, False)
    for index in range(8):
        count = gathered * BLK
        if index in (2, 3):
            count = sum(parts_of(g)[index - 2][1] for g in GATHERED)
        rows_wait(ag_send.at[index], count, False)
    remote(psend, precv, p_send, p_send, partner).wait_send()
    remote(t1, u1, r1_send, r1_send, partner).wait_send()
    remote(t2, u2, r2_send, r2_send, partner).wait_send()
    wait_slabs(y_send, EXPERTS - 1, False)


def body(tokens, norm_gain, expert_ids, route_weight, w_gate, w_up, w_down):
    vmem = pl.BlockSpec(memory_space=pltpu.VMEM)
    hbm = pl.BlockSpec(memory_space=pl.ANY)
    dma = pltpu.SemaphoreType.DMA
    return pl.pallas_call(
        main_kernel,
        out_shape=jax.ShapeDtypeStruct((TOK, DQ), BF16),
        in_specs=[hbm, vmem, vmem, vmem, hbm, hbm, hbm],
        out_specs=vmem,
        scratch_shapes=[
            pltpu.VMEM((TOK, D), BF16),
            pltpu.VMEM((TOK, D), BF16),
            pltpu.VMEM((max(NF, 1) * NY, NX, SLAB, LANES), BF16),
            pltpu.VMEM((max(NF, 1) * NY, NX, SLAB, LANES), BF16),
            pltpu.VMEM((EXPERTS, SLAB, LANES), BF16),
            pltpu.VMEM((EXPERTS, SLAB, LANES), BF16),
            pltpu.VMEM((ALL_ROWS, TOK), BF16),
            pltpu.VMEM((ALL_ROWS, TOK), BF16),
            pltpu.VMEM((NT, D, 2 * LANES), BF16),
            pltpu.VMEM((BLOCK_H, D), BF16),
            pltpu.VMEM((2 * ALL_ROWS, D), BF16),
            pltpu.VMEM((2, TOP_ROWS, 2 * LANES), F32),
            pltpu.VMEM((TOP_ROWS, BLOCK_H), BF16),
            pltpu.VMEM((ALL_ROWS, DQ), F32),
            pltpu.VMEM((EXPERTS * SLAB, LANES), F32),
            pltpu.VMEM((4, ALL_ROWS, DQ), F32),
            pltpu.VMEM((4, ALL_ROWS, DQ), BF16),
            pltpu.VMEM((4, ALL_ROWS, DQ), BF16),
            pltpu.VMEM((ALL_ROWS, DQ), BF16),
            pltpu.VMEM((ALL_ROWS, DQ), BF16),
            pltpu.VMEM((2, ALL_ROWS, DQ), BF16),
            pltpu.VMEM((2, ALL_ROWS, DQ), BF16),
            pltpu.VMEM((EXPERTS, SLAB, LANES), BF16),
            pltpu.VMEM((EXPERTS, SLAB, LANES), BF16),
            pltpu.VMEM((TOK, DQ), F32),
            dma,
            dma((2,)),
            dma,
            dma,
            dma((NG,)),
            dma((9,)),
            dma((NG, 4)),
            dma,
            dma((NG, 4)),
            dma,
            dma((NG, 2)),
            dma,
            dma((NG,)),
            dma,
            dma((NG,)),
        ],
        compiler_params=pltpu.CompilerParams(
            collective_id=0, has_side_effects=True, vmem_limit_bytes=VMEM_BYTES
        ),
    )(tokens, norm_gain.reshape(1, D), expert_ids.T, route_weight.T, w_gate, w_up, w_down)


def solution(mesh):
    in_specs = (
        P("ep", None),
        P(),
        P("ep", None),
        P("ep", None),
        P("ep", None, "tp"),
        P("ep", None, "tp"),
        P("ep", "tp", None),
    )
    return jax.shard_map(
        body, mesh=mesh, in_specs=in_specs, out_specs=P("ep", "tp"), check_vma=False
    )
```

```python
import jax
import jax.numpy as jnp
from jax import lax
from jax.experimental import pallas as pl
from jax.experimental.pallas import tpu as pltpu
from jax.sharding import PartitionSpec as P

MESH = pl.DeviceIdType.MESH
F32, BF16, I32 = jnp.float32, jnp.bfloat16, jnp.int32
EPSILON = 1e-05

NZ, NY, NX = 8, 4, 4
EXPERTS = NZ * NY
TOK = 256
D = 2048
CAP = 20
LANES = 128
DQ = D // NX
NJ = DQ // LANES
SLAB = CAP * NJ
BLOCK_H = 896
NT = BLOCK_H // LANES
BLK = NY * CAP

GROUPS = ((0,), (2, 6), (4,), (5, 3), (1,), (7,))
ISSUE = (1, 0, 2, 3, 5, 4)
WHOLE = (0, 4, 5)
EARLY = 3
COMBINE = (0, 1, 2, 3, 4, 5)
ORDER = (
    ("start", 1),
    ("send", 3),
    ("start", 0),
    ("weights",),
    ("ready", 0),
    ("up", 0, 0),
    ("send", 5),
    ("up", 0, 1),
    ("up", 0, 2),
    ("send", 4),
    ("start", 2),
    ("up", 0, 3),
    ("down", 0, 0),
    ("down", 0, 1),
    ("down", 0, 2),
    ("down", 0, 3),
    ("forward", 1),
    ("first", 0),
    ("forward", 2),
    ("start", 3),
    ("finish", 1),
    ("second", 0),
    ("ready", 1),
    ("up", 1, 0),
    ("finish", 2),
    ("up", 1, 1),
    ("up", 1, 2),
    ("up", 1, 3),
    ("down", 1, 0),
    ("forward", 3),
    ("down", 1, 1),
    ("down", 1, 2),
    ("down", 1, 3),
    ("first", 1),
    ("last", 0),
    ("ready", 2),
    ("up", 2, 0),
    ("up", 2, 1),
    ("up", 2, 2),
    ("up", 2, 3),
    ("down", 2, 0),
    ("down", 2, 1),
    ("finish", 3),
    ("down", 2, 2),
    ("down", 2, 3),
    ("start", 5),
    ("start", 4),
    ("first", 2),
    ("ready", 3),
    ("up", 3, 0),
    ("second", 1),
    ("up", 3, 1),
    ("up", 3, 2),
    ("up", 3, 3),
    ("second", 2),
    ("down", 3, 0),
    ("down", 3, 1),
    ("down", 3, 2),
    ("down", 3, 3),
    ("first", 3),
    ("ready", 4),
    ("up", 4, 0),
    ("up", 4, 1),
    ("last", 1),
    ("up", 4, 2),
    ("up", 4, 3),
    ("down", 4, 0),
    ("last", 2),
    ("down", 4, 1),
    ("down", 4, 2),
    ("down", 4, 3),
    ("first", 4),
    ("ready", 5),
    ("up", 5, 0),
    ("second", 3),
    ("up", 5, 1),
    ("up", 5, 2),
    ("up", 5, 3),
    ("down", 5, 0),
    ("down", 5, 1),
    ("down", 5, 2),
    ("down", 5, 3),
    ("first", 5),
    ("second", 4),
    ("last", 3),
    ("second", 5),
    ("last", 4),
    ("mix", 0),
    ("mix", 1),
    ("mix", 2),
    ("last", 5),
    ("mix", 3),
    ("mix", 4),
    ("mix", 5),
)
NG = len(GROUPS)
OFFSETS = tuple(dz for offsets in GROUPS for dz in offsets)
BASE = tuple(sum(len(o) for o in GROUPS[:g]) for g in range(NG))
SIZE = tuple(len(o) for o in GROUPS)
NF = len(WHOLE)
GATHERED = tuple(g for g in range(NG) if g not in WHOLE)
TOP_ROWS = 2 * BLK * max(SIZE)
CUTS = (0, 2, 4, 6, 7)
QUARTERS = (2, 1, 3, 0)
ALL_ROWS = EXPERTS * CAP
VMEM_BYTES = 53 * 1024 * 1024 + 512 * 1024


def main_kernel(
    tok_hbm, gain_ref, ids_ref, weight_ref, wg_hbm, wu_hbm, wd_hbm, result,
    tok, normed, full_slabs, full_in, out_slabs, arrived, mix_hi, mix_lo,
    wgu, wd, routed, acc, hidden, rows, whole_rows, slabs,
    own, psend, precv, t1, u1, t2, u2, ysend, back, total,
    tok_sem, w_sem, f_send, d_send, d_recv, ag_send, ag_recv, p_send, p_recv,
    r1_send, r1_recv, r2_send, r2_recv, y_send, y_recv,
):
    x = lax.axis_index("tp")
    ep = lax.axis_index("ep")
    core = lax.rem(ep, 2)
    expert = ep // 2
    y = lax.rem(expert, NY)
    z = expert // NY
    right, left = {"tp": lax.rem(x + 1, NX)}, {"tp": lax.rem(x + NX - 1, NX)}
    partner = {"ep": ep + 1 - 2 * core}

    def chip(to_z, to_y):
        return {"ep": (to_z * NY + to_y) * 2 + core}

    def remote(src, dst, send, recv, device):
        return pltpu.make_async_remote_copy(
            src_ref=src, dst_ref=dst, send_sem=send, recv_sem=recv,
            device_id=device, device_id_type=MESH,
        )

    def weight_copies():
        copies = []
        for n in range(NT):
            tile = pl.ds(n * LANES, LANES)
            for k, w in enumerate((wg_hbm, wu_hbm)):
                copies.append(
                    pltpu.make_async_copy(
                        w.at[0, :, tile], wgu.at[n, :, pl.ds(k * LANES, LANES)], w_sem.at[0]
                    )
                )
        copies.append(pltpu.make_async_copy(wd_hbm.at[0], wd, w_sem.at[1]))
        return copies

    tok_copy = pltpu.make_async_copy(tok_hbm, tok, tok_sem)
    tok_copy.start()

    barrier = pltpu.get_barrier_semaphore()

    def greet(i, carry):
        other = lax.rem(expert + i, EXPERTS)
        pl.semaphore_signal(
            barrier, inc=1, device_id={"ep": other * 2 + core}, device_id_type=MESH
        )
        return carry

    lax.fori_loop(1, EXPERTS, greet, 0)
    for device in (right, left, partner):
        pl.semaphore_signal(barrier, inc=1, device_id=device, device_id_type=MESH)
    for copy in weight_copies():
        copy.start()

    def rows_wait(sem, count, recv):
        copy = remote(t1.at[pl.ds(0, count)], u1.at[pl.ds(0, count)], sem, sem, partner)
        copy.wait_recv() if recv else copy.wait_send()

    def quarter_columns(q):
        return pl.ds(pl.multiple_of(q * DQ, DQ), DQ)

    def to_slabs(src, src_row, dst, dst_row, count):
        for i in range(count):
            for j in range(NJ):
                dst[pl.ds(dst_row + i * SLAB + j * CAP, CAP), :] = src[
                    pl.ds(src_row + i * CAP, CAP), pl.ds(j * LANES, LANES)
                ]

    ids = [ids_ref[k : k + 1, :] for k in range(2)]
    experts = lax.broadcasted_iota(I32, (EXPERTS, TOK), 0)
    named = [experts == ids[k] for k in range(2)]
    counts = (named[0].astype(F32) + named[1].astype(F32)).astype(BF16)
    token_from = lax.broadcasted_iota(I32, (TOK, TOK), 0)
    token_to = lax.broadcasted_iota(I32, (TOK, TOK), 1)
    earlier = jnp.where(token_from < token_to, 1.0, 0.0).astype(BF16)
    before = jnp.dot(counts, earlier, preferred_element_type=F32)
    place = []
    for k in range(2):
        slot = jnp.sum(jnp.where(named[k], before, 0.0), axis=0, keepdims=True).astype(I32)
        away = ((ids[k] >> 2) + (NZ - z)) & (NZ - 1)
        position = jnp.zeros_like(away)
        for at, dz in enumerate(OFFSETS):
            position = jnp.where(away == dz, at, position)
        place.append((position * NY + (ids[k] & (NY - 1))) * CAP + slot)
    row_index = lax.broadcasted_iota(I32, (ALL_ROWS, TOK), 0)
    hits = [row_index == place[k] for k in range(2)]
    chosen = jnp.where(hits[0] | hits[1], 1.0, 0.0).astype(BF16)

    tok_copy.wait()
    values = tok[...].astype(F32)
    center = values - jnp.mean(values, axis=-1, keepdims=True)
    spread = jnp.mean(center * center, axis=-1, keepdims=True)
    normed[...] = (center * lax.rsqrt(spread + EPSILON) * gain_ref[...]).astype(BF16)

    rows[...] = jnp.dot(chosen, normed[:, quarter_columns(x)], preferred_element_type=F32)
    pl.semaphore_wait(barrier, EXPERTS - 1 + 3)

    def prepare(g):
        if g in WHOLE:
            at = WHOLE.index(g) * NY
            near = chosen[BASE[g] * BLK : (BASE[g] + 1) * BLK]
            for q in range(NX):
                part = pl.ds(q * BLK, BLK)
                whole_rows[part] = jnp.dot(
                    near, normed[:, q * DQ : (q + 1) * DQ], preferred_element_type=F32
                )
                to_slabs(whole_rows, q * BLK, slabs, q * NY * SLAB, NY)
                full_slabs[at : at + NY, q] = (
                    slabs[q * NY * SLAB : (q + 1) * NY * SLAB]
                    .reshape(NY, SLAB, LANES)
                    .astype(BF16)
                )
            return
        first_slab, count = BASE[g] * NY, SIZE[g] * NY
        to_slabs(rows, first_slab * CAP, slabs, first_slab * SLAB, count)
        out_slabs[pl.ds(first_slab, count)] = (
            slabs[pl.ds(first_slab * SLAB, count * SLAB)].reshape(count, SLAB, LANES).astype(BF16)
        )

    def dispatch(g):
        for d, dz in enumerate(GROUPS[g]):
            for dy in range(NY):
                to_y = lax.rem(y + dy, NY)
                if g in WHOLE:
                    at = WHOLE.index(g) * NY
                    src, dst, sent = full_slabs, full_in, f_send
                else:
                    at = (BASE[g] + d) * NY
                    src, dst, sent = out_slabs, arrived, d_send
                if dy or dz:
                    remote(
                        src.at[at + to_y], dst.at[at + y], sent, d_recv.at[g],
                        chip(lax.rem(z + dz, NZ), to_y),
                    ).start()
                else:
                    dst[at + y] = src[at + y]

    for g in ISSUE[:EARLY]:
        prepare(g)
        dispatch(g)
    for g in ISSUE[EARLY:]:
        prepare(g)

    mix = jnp.where(hits[0], weight_ref[0:1, :], 0.0) + jnp.where(hits[1], weight_ref[1:2, :], 0.0)
    high = mix.astype(BF16)
    mix_hi[...] = high
    mix_lo[...] = (mix - high.astype(F32)).astype(BF16)

    def wait_slabs(sem, count, recv):
        span = pl.ds(0, count)
        copy = remote(out_slabs.at[span], back.at[span], sem, sem, partner)
        copy.wait_recv() if recv else copy.wait_send()

    q_own, q_left, q_right, q_far = (
        x, lax.rem(x + NX - 1, NX), lax.rem(x + 1, NX), lax.rem(x + 2, NX)
    )

    def parts_of(g):
        count = SIZE[g] * BLK
        cut = -(-count // 32) * 16
        return (0, cut), (cut, count - cut)

    def shared(g, part):
        return pl.ds(BASE[g] * BLK + part[0], part[1])

    def gather_rows(g, part, other):
        start = BASE[g] * 2 * BLK + (SIZE[g] * BLK if other else 0)
        return pl.ds(start + part[0], part[1])

    def gather_copy(g, index):
        whole = (0, SIZE[g] * BLK)
        first, second = parts_of(g)
        q, part, device = (
            (q_own, whole, right),
            (q_own, whole, left),
            (q_left, first, right),
            (q_right, second, left),
            (q_own, whole, partner),
            (q_left, whole, partner),
            (q_right, whole, partner),
            (q_far, whole, partner),
        )[index]
        columns = pl.ds(0, D) if g in WHOLE else quarter_columns(q)
        src = routed.at[gather_rows(g, part, False), columns]
        dst = routed.at[gather_rows(g, part, index >= 4), columns]
        sent = 8 if g in WHOLE else index
        return remote(src, dst, ag_send.at[sent], ag_recv.at[g, (0, 1, 2, 2, 3, 3, 3, 3)[index]], device)

    def gather_start(g):
        if g in WHOLE:
            at = WHOLE.index(g) * NY
            wait_slabs(d_recv.at[g], (NY - (0 in GROUPS[g])) * NX, True)
            for q in range(NX):
                slabs[0 : NY * SLAB] = (
                    full_in[at : at + NY, q].reshape(NY * SLAB, LANES).astype(F32)
                )
                for i in range(NY):
                    for j in range(NJ):
                        rows[pl.ds(i * CAP, CAP), pl.ds(j * LANES, LANES)] = slabs[
                            pl.ds(i * SLAB + j * CAP, CAP), :
                        ]
                routed[gather_rows(g, (0, BLK), False), q * DQ : (q + 1) * DQ] = rows[
                    0:BLK
                ].astype(BF16)
            gather_copy(g, 4).start()
            return
        count = SIZE[g] * NY
        wait_slabs(d_recv.at[g], count - (0 in GROUPS[g]), True)
        span = pl.ds(BASE[g] * NY, count)
        slabs[0 : count * SLAB] = arrived[span].reshape(count * SLAB, LANES).astype(F32)
        for i in range(count):
            for j in range(NJ):
                rows[pl.ds(i * CAP, CAP), pl.ds(j * LANES, LANES)] = slabs[
                    pl.ds(i * SLAB + j * CAP, CAP), :
                ]
        routed[gather_rows(g, (0, count * CAP), False), quarter_columns(q_own)] = rows[
            0 : count * CAP
        ].astype(BF16)
        for index in (0, 1, 4):
            gather_copy(g, index).start()

    def gather_forward(g):
        gather_copy(g, 0).wait_recv()
        gather_copy(g, 2).start()
        gather_copy(g, 5).start()
        gather_copy(g, 1).wait_recv()
        gather_copy(g, 3).start()
        gather_copy(g, 6).start()

    def gather_finish(g):
        rows_wait(ag_recv.at[g, 2], SIZE[g] * BLK, True)
        gather_copy(g, 7).start()

    def gather_partner(g):
        span = gather_rows(g, (0, SIZE[g] * BLK), True)
        remote(
            routed.at[span], routed.at[span], ag_send.at[8], ag_recv.at[g, 3], partner
        ).wait_recv()

    def up_part(g, part):
        count = 2 * SIZE[g] * BLK
        span = pl.ds(BASE[g] * 2 * BLK, count)

        def activate(n):
            gate, up = acc[n % 2, 0:count, 0:LANES], acc[n % 2, 0:count, LANES:]
            value = gate / (1.0 + jnp.exp(-gate)) * up
            hidden[0:count, n * LANES : (n + 1) * LANES] = value.astype(BF16)

        for n in range(CUTS[part], CUTS[part + 1]):
            if n:
                activate(n - 1)
            acc[n % 2, 0:count] = jnp.dot(routed[span], wgu[n], preferred_element_type=F32)
        if CUTS[part + 1] == NT:
            activate(NT - 1)

    def partial_copy(g, k):
        span = shared(g, (0, SIZE[g] * BLK))
        return remote(
            psend.at[k, span], precv.at[k, span], p_send, p_recv.at[g, k], partner
        )

    def down_part(g, k):
        count = SIZE[g] * BLK
        span = shared(g, (0, count))
        value = jnp.dot(
            hidden[0 : 2 * count], wd[:, quarter_columns(lax.rem(x + QUARTERS[k], NX))],
            preferred_element_type=F32,
        )
        psend[k, span] = value[count:].astype(BF16)
        own[k, span] = value[:count]
        partial_copy(g, k).start()

    def first_copy(g, way):
        span = shared(g, parts_of(g)[way])
        return remote(
            t1.at[span], u1.at[span], r1_send, r1_recv.at[g, way], (right, left)[way]
        )

    def second_copy(g, way):
        span = shared(g, (0, SIZE[g] * BLK))
        return remote(
            t2.at[way, span], u2.at[way, span], r2_send, r2_recv.at[g],
            (right, left)[way],
        )

    def chip_sum(k, span):
        return own[k, span] + precv[k, span].astype(F32)

    def reduce_first(g):
        partial_copy(g, 0).wait_recv()
        span = shared(g, (0, SIZE[g] * BLK))
        t1[span] = chip_sum(0, span).astype(BF16)
        for way in range(2):
            first_copy(g, way).start()

    def reduce_second(g):
        for way in range(2):
            added, plain = (shared(g, parts_of(g)[p]) for p in (way, 1 - way))
            partial_copy(g, 1 + way).wait_recv()
            t2[way, plain] = chip_sum(1 + way, plain).astype(BF16)
            first_copy(g, way).wait_recv()
            t2[way, added] = (chip_sum(1 + way, added) + u1[added].astype(F32)).astype(BF16)
            second_copy(g, way).start()

    def reduce_last(g):
        count = SIZE[g] * BLK
        span = shared(g, (0, count))
        partial_copy(g, 3).wait_recv()
        remote(
            t2.at[:, span], u2.at[:, span], r2_send, r2_recv.at[g], partner
        ).wait_recv()
        rows[0:count] = chip_sum(3, span) + u2[0, span].astype(F32) + u2[1, span].astype(F32)
        for i in range(SIZE[g] * NY):
            for j in range(NJ):
                slabs[pl.ds(i * SLAB + j * CAP, CAP), :] = rows[
                    pl.ds(i * CAP, CAP), pl.ds(j * LANES, LANES)
                ]
        ysend[pl.ds(BASE[g] * NY, SIZE[g] * NY)] = (
            slabs[0 : SIZE[g] * NY * SLAB].reshape(SIZE[g] * NY, SLAB, LANES).astype(BF16)
        )
        for d, dz in enumerate(GROUPS[g]):
            at = (BASE[g] + d) * NY
            for dy in range(NY):
                to_y = lax.rem(y + dy, NY)
                if dz == 0 and dy == 0:
                    back[at + y] = ysend[at + y]
                    continue
                remote(
                    ysend.at[at + to_y], back.at[at + y], y_send, y_recv.at[g],
                    chip(lax.rem(z + NZ - dz, NZ), to_y),
                ).start()

    def combine(g):
        count = SIZE[g] * NY
        wait_slabs(y_recv.at[g], count - (0 in GROUPS[g]), True)
        slabs[0 : count * SLAB] = (
            back[pl.ds(BASE[g] * NY, count)].reshape(count * SLAB, LANES).astype(F32)
        )
        for i in range(count):
            for j in range(NJ):
                rows[pl.ds(i * CAP, CAP), pl.ds(j * LANES, LANES)] = slabs[
                    pl.ds(i * SLAB + j * CAP, CAP), :
                ]
        picked = rows[0 : count * CAP].astype(BF16)
        span = pl.ds(BASE[g] * BLK, count * CAP)
        value = sum(
            lax.dot_general(
                mix[span], picked, (((0,), (0,)), ((), ())), preferred_element_type=F32
            )
            for mix in (mix_hi, mix_lo)
        )
        if g == COMBINE[0]:
            total[...] = value
        elif g != COMBINE[-1]:
            total[...] += value
        else:
            result[...] = (total[...] + value).astype(BF16)

    def weights_wait():
        pltpu.make_async_copy(wgu, wgu, w_sem.at[0]).wait()
        pltpu.make_async_copy(wd, wd, w_sem.at[1]).wait()

    steps = {
        "send": dispatch,
        "start": gather_start,
        "forward": gather_forward,
        "finish": gather_finish,
        "weights": weights_wait,
        "ready": gather_partner,
        "up": up_part,
        "down": down_part,
        "first": reduce_first,
        "second": reduce_second,
        "last": reduce_last,
        "mix": combine,
    }
    for name, *which in ORDER:
        steps[name](*which)

    if NF:
        span = pl.ds(0, NF * NY - (0 in [GROUPS[g][0] for g in WHOLE]))
        remote(full_slabs.at[span], full_in.at[span], f_send, f_send, partner).wait_send()
        span = pl.ds(0, NF * BLK)
        remote(
            routed.at[span], routed.at[span], ag_send.at[8], ag_send.at[8], partner
        ).wait_send()
    gathered = sum(SIZE[g] for g in GATHERED)
    own_sent = 0 in [dz for g in GATHERED for dz in GROUPS[g]]
    wait_slabs(d_send, gathered * NY - own_sent, False)
    for index in range(8):
        count = gathered * BLK
        if index in (2, 3):
            count = sum(parts_of(g)[index - 2][1] for g in GATHERED)
        rows_wait(ag_send.at[index], count, False)
    remote(psend, precv, p_send, p_send, partner).wait_send()
    remote(t1, u1, r1_send, r1_send, partner).wait_send()
    remote(t2, u2, r2_send, r2_send, partner).wait_send()
    wait_slabs(y_send, EXPERTS - 1, False)


def body(tokens, norm_gain, expert_ids, route_weight, w_gate, w_up, w_down):
    vmem = pl.BlockSpec(memory_space=pltpu.VMEM)
    hbm = pl.BlockSpec(memory_space=pl.ANY)
    dma = pltpu.SemaphoreType.DMA
    return pl.pallas_call(
        main_kernel,
        out_shape=jax.ShapeDtypeStruct((TOK, DQ), BF16),
        in_specs=[hbm, vmem, vmem, vmem, hbm, hbm, hbm],
        out_specs=vmem,
        scratch_shapes=[
            pltpu.VMEM((TOK, D), BF16),
            pltpu.VMEM((TOK, D), BF16),
            pltpu.VMEM((max(NF, 1) * NY, NX, SLAB, LANES), BF16),
            pltpu.VMEM((max(NF, 1) * NY, NX, SLAB, LANES), BF16),
            pltpu.VMEM((EXPERTS, SLAB, LANES), BF16),
            pltpu.VMEM((EXPERTS, SLAB, LANES), BF16),
            pltpu.VMEM((ALL_ROWS, TOK), BF16),
            pltpu.VMEM((ALL_ROWS, TOK), BF16),
            pltpu.VMEM((NT, D, 2 * LANES), BF16),
            pltpu.VMEM((BLOCK_H, D), BF16),
            pltpu.VMEM((2 * ALL_ROWS, D), BF16),
            pltpu.VMEM((2, TOP_ROWS, 2 * LANES), F32),
            pltpu.VMEM((TOP_ROWS, BLOCK_H), BF16),
            pltpu.VMEM((ALL_ROWS, DQ), F32),
            pltpu.VMEM((NX * BLK, DQ), F32),
            pltpu.VMEM((EXPERTS * SLAB, LANES), F32),
            pltpu.VMEM((4, ALL_ROWS, DQ), F32),
            pltpu.VMEM((4, ALL_ROWS, DQ), BF16),
            pltpu.VMEM((4, ALL_ROWS, DQ), BF16),
            pltpu.VMEM((ALL_ROWS, DQ), BF16),
            pltpu.VMEM((ALL_ROWS, DQ), BF16),
            pltpu.VMEM((2, ALL_ROWS, DQ), BF16),
            pltpu.VMEM((2, ALL_ROWS, DQ), BF16),
            pltpu.VMEM((EXPERTS, SLAB, LANES), BF16),
            pltpu.VMEM((EXPERTS, SLAB, LANES), BF16),
            pltpu.VMEM((TOK, DQ), F32),
            dma,
            dma((2,)),
            dma,
            dma,
            dma((NG,)),
            dma((9,)),
            dma((NG, 4)),
            dma,
            dma((NG, 4)),
            dma,
            dma((NG, 2)),
            dma,
            dma((NG,)),
            dma,
            dma((NG,)),
        ],
        compiler_params=pltpu.CompilerParams(
            collective_id=0, has_side_effects=True, vmem_limit_bytes=VMEM_BYTES
        ),
    )(tokens, norm_gain.reshape(1, D), expert_ids.T, route_weight.T, w_gate, w_up, w_down)


def solution(mesh):
    in_specs = (
        P("ep", None),
        P(),
        P("ep", None),
        P("ep", None),
        P("ep", None, "tp"),
        P("ep", None, "tp"),
        P("ep", "tp", None),
    )
    return jax.shard_map(
        body, mesh=mesh, in_specs=in_specs, out_specs=P("ep", "tp"), check_vma=False
    )
```
